512 devices in a mesh: ep: 32 (over z, core), tp: 16 (over y, x).
Axes of the slice: x: 4, y: 4, z: 16, core: 2. Of those that a mesh axis runs over, the one named last changes fastest.
Arguments:
- tokens: bfloat16 [512, 2048], P('ep'), may hold values from -6 to 6
- norm_gain: float32 [2048], replicated, may hold values from 0.1 to 1.9
- w_query: bfloat16 [2048, 2048], P('ep', 'tp'), may hold values from -0.125 to 0.125
- w_key: bfloat16 [2048, 2048], P('ep', 'tp'), may hold values from -0.125 to 0.125
- w_decay: bfloat16 [2048, 2048], P('ep', 'tp'), may hold values from -0.125 to 0.125
- w_value: bfloat16 [2048, 4096], P('ep', 'tp'), may hold values from -0.125 to 0.125
- w_outgate: bfloat16 [2048, 4096], P('ep', 'tp'), may hold values from -0.125 to 0.125
- decay_rate: float32 [2048], P('tp'), may hold values from 0.02 to 1
- state: float32 [512, 16, 128, 256], P('ep', 'tp'), may hold values from -15 to 15
- head_gain: float32 [256], replicated, may hold values from 0.1 to 1.9
- w_output: bfloat16 [4096, 2048], P('tp'), may hold values from -0.09375 to 0.09375
- moe_gain: float32 [2048], replicated, may hold values from 0.1 to 1.9
- expert_ids: int32 [512, 2], P('ep'), may hold values from 0 to 31, all different within a row; in each aligned block of 16 rows (0 to 15, 16 to 31, ...) at most 2 rows name the same one
- group_prob: float32 [512], P('ep'), may hold values from 0.3 to 1
- inner_prob: float32 [512, 2], P('ep'), may hold values from 0.05 to 1
- w_gate: bfloat16 [32, 2048, 2048], P('ep', None, 'tp'), may hold values from -0.125 to 0.125
- w_up: bfloat16 [32, 2048, 2048], P('ep', None, 'tp'), may hold values from -0.125 to 0.125
- w_down: bfloat16 [32, 2048, 2048], P('ep', 'tp'), may hold values from -0.125 to 0.125
Outputs:
- output: bfloat16 [512, 2048], P('ep', 'tp')
The draws below stay inside these ranges and needn't reach their ends.
Inputs may be any that keep to these rules, and one draw needn't show every extreme that they name: `expert_ids`: the 2 experts of a token differ. In the rows of one index of ep no expert is named more than 2 times, a bound that some block reaches there.
All inputs are finite; a program needn't handle non-finite values.
Results may differ from the reference program's by a relative error of at most 0.025.
Values may be sent and summed in bfloat16 or wider, within the bound.
A program may use at most 64 MiB of HBM per device.

```python
import math
import jax
import jax.numpy as jnp
import numpy as np
from jax import lax

D = 2048
DK = 128
DV = 256
GLA_HEADS = 16
FF = 2048
TOP = 2
SEQ_DEV = 16
SEQS = 512
EXPERTS = 32
CAP = 2
FF_BLOCK = 128
N_TP = 16


def shard_levels(key, shape, shards, low, top_value):
    def one(axis_at, shards_of):
        heights = jax.random.uniform(jax.random.fold_in(jax.random.fold_in(key, 6), axis_at), (shards_of,), jnp.float32, low / len(shards), top_value / len(shards))
        return jnp.repeat(jnp.exp(heights), shape[axis_at] // shards_of).reshape((-1,) + (1,) * (len(shape) - axis_at - 1))

    level = one(*shards[0])
    for cut in shards[1:]:
        level = level * one(*cut)
    return level


def routed_block(own_key, own, number, rows, amount, top, bound, lean):
    sequence = jax.random.permutation(own_key, amount)
    heavy_load, usual = shares(amount, rows * top, bound, lean, True), shares(amount, rows * top, bound, lean, False)
    places = jnp.arange(amount)

    def named(sizes, rotation):
        used = int((sizes > 0).sum())
        fixed = max(1, used // 4)
        passed = fixed + (places - fixed + rotation * (used - fixed)) % max(1, amount - fixed)
        return jnp.zeros((amount,), jnp.int32).at[sequence[jnp.where(places < fixed, places, passed)]].set(jnp.asarray(sizes, jnp.int32))

    sizes = jnp.where(number % 4 == 0, named(heavy_load, number // 4), named(usual, number - number // 4 - 1))
    mixed = jax.random.permutation(jax.random.fold_in(own, 3), amount)
    source_of, receiver = mixed[0:amount // 2 * 2:2], mixed[1:amount // 2 * 2:2]
    slack = jnp.minimum(sizes[source_of] - 1, bound - sizes[receiver]) // 2
    slack = jnp.where((source_of == sequence[0]) | (receiver == sequence[0]) | (sizes[receiver] == 0), 0, jnp.maximum(slack, 0))
    passed = jax.random.randint(jax.random.fold_in(own, 4), (amount // 2,), 0, 1 << 20) % (slack + 1)
    sizes = sizes.at[source_of].add(-passed).at[receiver].add(passed)
    items = jnp.searchsorted(jnp.cumsum(sizes), jnp.arange(rows * top), side="right").astype(jnp.int32)
    listing = items.reshape(top, rows).T
    listing = listing[jax.random.permutation(jax.random.fold_in(own, 1), rows)]
    rotation = jax.random.randint(jax.random.fold_in(own, 2), (rows, 1), 0, top)
    return jnp.take_along_axis(listing, (jnp.arange(top)[None, :] + rotation) % top, axis=1)


def shares(count, total, reach, skew, full):
    weights = [(1 << 20) // math.isqrt(standing ** skew) + 1 for standing in range(1, count + 1)]
    largest = reach if full else min(reach, max(-(-total // count), total * weights[0] // sum(weights)))
    least = 1 if total - largest >= count - 1 else 0
    holding, rest = [largest] + [least] * (count - 1), total - largest - least * (count - 1)
    while rest > 0:
        movable = [i for i in range(1, count) if holding[i] < largest] or [i for i in range(1, count) if holding[i] < reach]
        mass, budget = sum([weights[i] for i in movable]), rest
        for i in movable:
            addition = min(reach - holding[i], max(1, budget * weights[i] // mass), rest)
            holding[i] = holding[i] + addition
            rest = rest - addition
    return np.array(holding)


def scatter_about(rng, extent, width, limit, split=(), kind=jnp.bfloat16):
    result = width * jax.random.normal(rng, extent, jnp.float32)
    if split:
        result = result * shard_levels(rng, extent, split, -0.22, 0.18)
    return jnp.clip(result, -limit, limit).astype(kind)


def setup_inputs(seed: int = 0) -> dict:
    streams_of = jax.random.split(jax.random.key(seed), 19)
    tokens = scatter_about(streams_of[0], (SEQS, D), 1.0, 6.0, ((0, 32),))
    norm_gain = jnp.clip(1.0 + 0.18 * jax.random.normal(streams_of[1], (D,), jnp.float32), 0.1, 1.9)
    w_query = scatter_about(streams_of[2], (D, GLA_HEADS * DK), D ** -0.5, 0.125, ((0, 32), (1, 16)))
    w_key = scatter_about(streams_of[3], (D, GLA_HEADS * DK), D ** -0.5, 0.125, ((0, 32), (1, 16)))
    w_decay = scatter_about(streams_of[4], (D, GLA_HEADS * DK), D ** -0.5, 0.125, ((0, 32), (1, 16)))
    w_value = scatter_about(streams_of[5], (D, GLA_HEADS * DV), D ** -0.5, 0.125, ((0, 32), (1, 16)))
    w_outgate = scatter_about(streams_of[6], (D, GLA_HEADS * DV), D ** -0.5, 0.125, ((0, 32), (1, 16)))
    decay_rate = jnp.clip(jnp.exp(math.log(1.0) - 3.912023 * jax.random.uniform(streams_of[7], (GLA_HEADS * DK,), jnp.float32) ** shard_levels(streams_of[7], (GLA_HEADS * DK,), ((0, 16),), -0.2, 0.2)), 0.02, 1.0)
    state = scatter_about(streams_of[8], (SEQS, GLA_HEADS, DK, DV), 3.0, 15.0, ((0, 32), (1, 16)), jnp.float32)
    head_gain = jnp.clip(1.0 + 0.18 * jax.random.normal(streams_of[9], (DV,), jnp.float32), 0.1, 1.9)
    w_output = scatter_about(streams_of[10], (GLA_HEADS * DV, D), (GLA_HEADS * DV) ** -0.5, 0.09375, ((0, 16),))
    moe_gain = jnp.clip(1.0 + 0.18 * jax.random.normal(streams_of[11], (D,), jnp.float32), 0.1, 1.9)
    expert_ids_keys = jax.random.split(jax.random.fold_in(streams_of[12], 1), SEQS // SEQ_DEV)
    expert_ids_turns = jax.random.permutation(jax.random.fold_in(streams_of[12], 3), SEQS // SEQ_DEV)
    expert_ids = jax.vmap(lambda own, number: routed_block(jax.random.fold_in(streams_of[12], 2), own, number, SEQ_DEV, EXPERTS, TOP, CAP, 2))(expert_ids_keys, expert_ids_turns).reshape((SEQS, TOP))
    group_prob = jnp.clip(0.3 + 0.7 * jax.random.uniform(streams_of[13], (SEQS,), jnp.float32) ** shard_levels(streams_of[13], (SEQS,), ((0, 32),), -0.2, 0.2), 0.3, 1.0)
    inner_prob = jnp.clip(0.05 + 0.95 * jax.random.uniform(streams_of[14], (SEQS, TOP), jnp.float32) ** shard_levels(streams_of[14], (SEQS, TOP), ((0, 32),), -0.2, 0.2), 0.05, 1.0)
    w_gate = scatter_about(streams_of[15], (EXPERTS, D, FF), D ** -0.5, 0.125, ((0, 32), (2, 16)))
    w_up = scatter_about(streams_of[16], (EXPERTS, D, FF), D ** -0.5, 0.125, ((0, 32), (2, 16)))
    w_down = scatter_about(streams_of[17], (EXPERTS, FF, D), FF ** -0.5, 0.125, ((0, 32), (1, 16)))
    return {"tokens": tokens, "norm_gain": norm_gain, "w_query": w_query, "w_key": w_key, "w_decay": w_decay, "w_value": w_value, "w_outgate": w_outgate, "decay_rate": decay_rate, "state": state, "head_gain": head_gain, "w_output": w_output, "moe_gain": moe_gain, "expert_ids": expert_ids, "group_prob": group_prob, "inner_prob": inner_prob, "w_gate": w_gate, "w_up": w_up, "w_down": w_down}


epsilon = 1e-05

def inverse_rms(values):
    return lax.rsqrt(lax.optimization_barrier(jnp.mean(values * values, axis=-1, keepdims=True)) + epsilon)

def reference(tokens, norm_gain, w_query, w_key, w_decay, w_value, w_outgate, decay_rate, state, head_gain, w_output, moe_gain, expert_ids, group_prob, inner_prob, w_gate, w_up, w_down):
    wide = jnp.float32
    narrow = jnp.bfloat16
    residual = tokens.astype(wide)
    normed = (residual * inverse_rms(residual) * norm_gain.astype(wide)).astype(narrow)

    def project(weight):
        return jnp.dot(normed, weight, preferred_element_type=wide)
    query = project(w_query).astype(narrow).astype(wide).reshape(SEQS, GLA_HEADS, DK) * DK ** (-0.5)
    key_rows = project(w_key).astype(narrow).astype(wide).reshape(SEQS, GLA_HEADS, DK)
    value_rows = project(w_value).astype(narrow).astype(wide).reshape(SEQS, GLA_HEADS, DV)
    gate_rows = project(w_outgate).astype(narrow).astype(wide).reshape(SEQS, GLA_HEADS, DV)
    decay_log = jax.nn.log_sigmoid(project(w_decay)) * decay_rate
    decay = jnp.exp(decay_log).reshape(SEQS, GLA_HEADS, DK)
    updated = decay[..., None] * state + key_rows[..., None] * value_rows[:, :, None, :]
    readout = jnp.einsum('shk,shkv->shv', query, updated, precision=lax.Precision.HIGHEST)
    gated = (readout * inverse_rms(readout) * head_gain.astype(wide) * jax.nn.silu(gate_rows)).astype(narrow)
    per_head = jnp.einsum('shv,hvd->shd', gated.astype(wide), w_output.astype(wide).reshape(GLA_HEADS, DV, D))
    attention = lax.optimization_barrier(jnp.sum(per_head.astype(narrow).astype(wide), axis=1))
    mixed = (residual + attention).astype(narrow)
    mixed_wide = mixed.astype(wide)
    moe_in = (mixed_wide * inverse_rms(mixed_wide) * moe_gain.astype(wide)).astype(narrow)
    route_weight = group_prob[:, None] * inner_prob / lax.optimization_barrier(jnp.sum(inner_prob, axis=1, keepdims=True))
    slot_total = EXPERTS * CAP

    def one_expert(total, inputs):
        weight_gate, weight_up, weight_down, index = inputs
        chosen = expert_ids == index
        coeff = lax.optimization_barrier(jnp.sum(jnp.where(chosen, route_weight, 0.0), axis=1))
        marks = jnp.where(jnp.any(chosen, axis=1), 0, 1).astype(jnp.int32)
        order = jnp.argsort(marks, stable=True)[:slot_total].astype(jnp.int32)
        rows = moe_in[order]
        gate = jnp.dot(rows, weight_gate, preferred_element_type=wide)
        upper = jnp.dot(rows, weight_up, preferred_element_type=wide)
        hidden = (jax.nn.silu(gate) * upper).astype(narrow)
        pieces = jnp.einsum('rbf,bfd->rbd', hidden.astype(wide).reshape(slot_total, N_TP, FF_BLOCK), weight_down.astype(wide).reshape(N_TP, FF_BLOCK, D))
        expert_out = lax.optimization_barrier(jnp.sum(pieces.astype(narrow).astype(wide), axis=1)).astype(narrow).astype(wide)
        total = total.at[order].add(coeff[order][:, None] * expert_out)
        return (total, None)
    experts_sum, _ = lax.scan(one_expert, jnp.zeros((SEQS, D), wide), (w_gate, w_up, w_down, jnp.arange(EXPERTS, dtype=jnp.int32)))
    return (mixed_wide + experts_sum).astype(narrow)
```

```python
import functools

import jax
import jax.numpy as jnp
from jax import lax
from jax.experimental import pallas as pl
from jax.experimental.pallas import tpu as pltpu
from jax.sharding import PartitionSpec as P

epsilon = 1e-05
MESH = pl.DeviceIdType.MESH
wide = jnp.float32
narrow = jnp.bfloat16


def kernel(
    E,
    T,
    tokens,
    norm_gain,
    w_query,
    w_key,
    w_decay,
    w_value,
    w_outgate,
    decay_rate,
    state,
    head_gain,
    w_output,
    moe_gain,
    expert_ids,
    group_prob,
    inner_prob,
    w_gate,
    w_up,
    w_down,
    out,
    wall,
    nbuf,
    acc,
    st_v,
    wo_v,
    wgu_v,
    wdn_v,
    head_send,
    head_recv,
    disp_send,
    disp_recv,
    rows_all,
    down_send,
    down_recv,
    ret_send,
    ret_recv,
    mixed_v,
    w_sem,
    big_sem,
    ring_send,
    d2d_send,
    ring_recv,
    d2d_recv,
    phase_send,
    phase_recv,
    rows_recv,
):
    Z = E // 2
    half = Z // 2
    S, D = tokens.shape
    KB = w_query.shape[0]
    CW = D // T
    QC = w_query.shape[1]
    VC = w_value.shape[1]
    FB = w_down.shape[0]
    DK = state.shape[1]
    e = lax.axis_index("ep")
    h = lax.axis_index("tp")
    z = e // 2
    c = e % 2
    own_rows = pl.ds(pl.multiple_of(c * KB, KB), KB)
    peer_rows = pl.ds(pl.multiple_of((1 - c) * KB, KB), KB)

    parts = (
        (w_query, 0, QC),
        (w_key, QC, QC),
        (w_value, 2 * QC, VC),
        (w_outgate, 2 * QC + VC, VC),
        (w_decay, 2 * QC + 2 * VC, QC),
    )
    loads = []
    for i, (ref, at, width) in enumerate(parts):
        loads.append(
            pltpu.make_async_copy(ref, wall.at[z, own_rows, pl.ds(at, width)], w_sem.at[i])
        )
        loads[-1].start()
    big = [
        pltpu.make_async_copy(state, st_v, big_sem.at[0]),
        pltpu.make_async_copy(w_output, wo_v, big_sem.at[1]),
        pltpu.make_async_copy(w_gate, wgu_v.at[:, pl.ds(0, FB)], big_sem.at[2]),
        pltpu.make_async_copy(w_up, wgu_v.at[:, pl.ds(FB, FB)], big_sem.at[3]),
        pltpu.make_async_copy(w_down, wdn_v, big_sem.at[4]),
    ]

    up_dev = (2 * ((z + 1) % Z) + c, h)
    down_dev = (2 * ((z + Z - 1) % Z) + c, h)
    peer = (2 * z + 1 - c, h)
    barrier = pltpu.get_barrier_semaphore()
    for dev in (up_dev, down_dev, peer):
        pl.semaphore_signal(barrier, inc=1, device_id=dev, device_id_type=MESH)

    def greet(i, _):
        pl.semaphore_signal(
            barrier, inc=1, device_id=(e, (h + i) % T), device_id_type=MESH
        )
        return 0

    lax.fori_loop(1, T, greet, 0)
    for copy in big:
        copy.start()

    residual = tokens[...].astype(wide)
    scale = lax.rsqrt(jnp.mean(residual * residual, axis=-1, keepdims=True) + epsilon)
    normed = (residual * scale * norm_gain[...]).astype(narrow)
    for i in range(Z):
        nbuf[i] = normed[:, 2 * KB * i : 2 * KB * (i + 1)]
    pl.semaphore_wait(barrier, 3 + T - 1)

    chunks = (
        (0, 2 * QC, (0, 1)),
        (2 * QC, VC, (2,)),
        (2 * QC + VC, VC, (3,)),
        (2 * QC + 2 * VC, QC, (4,)),
    )
    whole = range(len(chunks))
    dirs = ((up_dev, -1, (0, 1)), (down_dev, 1, (2, 3)))

    def block(zz, rows, ch):
        return wall.at[zz, rows, pl.ds(chunks[ch][0], chunks[ch][1])]

    def ring_copy(d, zz, s, ch):
        return pltpu.make_async_remote_copy(
            src_ref=block(zz, own_rows, ch),
            dst_ref=block(zz, own_rows, ch),
            send_sem=ring_send.at[d, s, ch],
            recv_sem=ring_recv.at[d, s, ch],
            device_id=dirs[d][0],
            device_id_type=MESH,
        )

    def peer_copy(d, zz, s, ch, rows):
        return pltpu.make_async_remote_copy(
            src_ref=block(zz, rows, ch),
            dst_ref=block(zz, rows, ch),
            send_sem=d2d_send.at[d, s, ch],
            recv_sem=d2d_recv.at[d, s, ch],
            device_id=peer,
            device_id_type=MESH,
        )

    def at_step(d, s):
        return (z + dirs[d][1] * s + 2 * Z) % Z

    def multiply(zz, ch):
        cols = slice(chunks[ch][0], chunks[ch][0] + chunks[ch][1])
        acc[:, cols] += jnp.dot(nbuf[zz], wall[zz, :, cols], preferred_element_type=wide)

    acc[...] = jnp.zeros_like(acc)
    for ch in whole:
        for i in chunks[ch][2]:
            loads[i].wait()
        for d in (0, 1):
            if half > 1 or ch in dirs[d][2]:
                ring_copy(d, z, 1, ch).start()
        peer_copy(0, z, 0, ch, own_rows).start()

    def step_of(s, first, before_last, last):
        for ch in whole:
            for d in (0, 1):
                if last and ch not in dirs[d][2]:
                    continue
                zz = at_step(d, s)
                ring_copy(d, zz, s, ch).wait_recv()
                if not last and (not before_last or ch in dirs[d][2]):
                    ring_copy(d, zz, s + 1, ch).start()
                peer_copy(d, zz, s, ch, own_rows).start()
            for d in (0,) if first else (0, 1):
                zz = at_step(d, s - 1)
                peer_copy(d, zz, s - 1, ch, peer_rows).wait_recv()
                multiply(zz, ch)

    if half > 1:
        step_of(1, True, half == 2, False)

        def middle(s, _):
            step_of(s, False, False, False)
            return 0

        if half > 3:
            lax.fori_loop(2, half - 1, middle, 0)
        elif half == 3:
            pass
        if half > 2:
            step_of(half - 1, False, True, False)
    step_of(half, half == 1, False, True)
    for d in (0, 1):
        for ch in dirs[d][2]:
            zz = at_step(d, half)
            peer_copy(d, zz, half, ch, peer_rows).wait_recv()
            multiply(zz, ch)

    def rounded(at, width):
        return acc[:, at : at + width].astype(narrow).astype(wide)

    query = rounded(0, QC) * DK ** (-0.5)
    key_rows = rounded(QC, QC)
    value_rows = rounded(2 * QC, VC)
    gate_rows = rounded(2 * QC + VC, VC)
    decay_pre = acc[:, 2 * QC + 2 * VC :]
    decay = jnp.exp(
        (jnp.minimum(decay_pre, 0.0) - jnp.log1p(jnp.exp(-jnp.abs(decay_pre)))) * decay_rate[...]
    )
    fresh = jnp.sum(query * key_rows, axis=1, keepdims=True) * value_rows
    turned = jnp.transpose(query * decay)
    big[0].wait()
    read = [
        jnp.sum(turned[:, i : i + 1] * st_v[i], axis=0, keepdims=True) for i in range(S)
    ]
    readout = jnp.concatenate(read, axis=0) + fresh
    size = lax.rsqrt(jnp.mean(readout * readout, axis=-1, keepdims=True) + epsilon)
    gated = (readout * size * head_gain[...] * jax.nn.silu(gate_rows)).astype(narrow)

    def whole_wait(ref, count, sem):
        pltpu.make_async_copy(ref.at[pl.ds(0, count)], ref.at[pl.ds(0, count)], sem).wait()

    def to_plane(src, dst, phase):
        def send(i, _):
            to = (h + i) % T
            pltpu.make_async_remote_copy(
                src_ref=src.at[to],
                dst_ref=dst.at[h],
                send_sem=phase_send.at[phase],
                recv_sem=phase_recv.at[phase],
                device_id=(e, to),
                device_id_type=MESH,
            ).start()
            return 0

        lax.fori_loop(1, T, send, 0)

    def to_column(src, dst, phase):
        def send(i, _):
            to = (e + i) % E
            pltpu.make_async_remote_copy(
                src_ref=src.at[to],
                dst_ref=dst.at[e],
                send_sem=phase_send.at[phase],
                recv_sem=phase_recv.at[phase],
                device_id=(to, h),
                device_id_type=MESH,
            ).start()
            return 0

        lax.fori_loop(1, E, send, 0)

    def in_slices(left, right_ref, dst):
        step = 2 if T % 2 == 0 else 1
        for i in range(0, T, step):
            both = jnp.dot(
                left, right_ref[:, i * CW : (i + step) * CW], preferred_element_type=wide
            ).astype(narrow)
            for j in range(step):
                dst[i + j] = both[:, j * CW : (j + 1) * CW]

    big[1].wait()
    in_slices(gated, wo_v, head_send)
    to_plane(head_send, head_recv, 0)
    head_recv[h] = head_send[h]

    ids = expert_ids[...]
    experts = lax.broadcasted_iota(jnp.int32, (S, E), 1)
    chosen = [ids[:, k : k + 1] == experts for k in range(ids.shape[1])]
    named = functools.reduce(jnp.logical_or, chosen)
    marks = jnp.where(named, 1.0, 0.0).astype(narrow)
    later = lax.broadcasted_iota(jnp.int32, (S, S), 0) > lax.broadcasted_iota(jnp.int32, (S, S), 1)
    rank = jnp.dot(
        jnp.where(later, 1.0, 0.0).astype(narrow), marks, preferred_element_type=wide
    ).astype(jnp.int32)
    inner = inner_prob[...]
    route = group_prob[...] * inner / jnp.sum(inner, axis=1, keepdims=True)
    weight = sum(jnp.where(m, route[:, k : k + 1], 0.0) for k, m in enumerate(chosen))
    per_slot = disp_send.shape[1]
    picked = [jnp.where(named & (rank == r), 1.0, 0.0) for r in range(per_slot)]
    picked_rows = [jnp.transpose(p).astype(narrow) for p in picked]

    whole_wait(head_recv, T - 1, phase_recv.at[0])
    attention = functools.reduce(jnp.add, [head_recv[i].astype(wide) for i in range(T)])
    own_cols = pl.ds(pl.multiple_of(h * CW, CW), CW)
    mixed = (tokens[:, own_cols].astype(wide) + attention).astype(narrow)
    mixed_v[...] = mixed.astype(wide)

    for r in range(per_slot):
        disp_send[:, r, :] = jnp.dot(picked_rows[r], mixed, preferred_element_type=wide)
    to_column(disp_send, disp_recv, 1)
    disp_recv[e] = disp_send[e]
    whole_wait(head_send, T - 1, phase_send.at[0])
    for i in (2, 3, 4):
        big[i].wait()
    whole_wait(disp_recv, E - 1, phase_recv.at[1])

    for r in range(per_slot):
        rows_all[h, r * E : (r + 1) * E, :] = disp_recv[:, r, :].astype(narrow)

    def rows_copy(i, to):
        return pltpu.make_async_remote_copy(
            src_ref=rows_all.at[i],
            dst_ref=rows_all.at[i],
            send_sem=phase_send.at[2],
            recv_sem=rows_recv.at[i],
            device_id=(e, to),
            device_id_type=MESH,
        )

    def spread(i, _):
        rows_copy(h, (h + i) % T).start()
        return 0

    lax.fori_loop(1, T, spread, 0)

    def gate_up(i, carry):
        total, squares = carry
        at = pl.multiple_of(i * CW, CW)
        x = rows_all[i].astype(wide)
        scaled = (x * moe_gain[:, pl.ds(at, CW)]).astype(narrow)
        total += jnp.dot(scaled, wgu_v[pl.ds(at, CW), :], preferred_element_type=wide)
        return total, squares + jnp.sum(x * x, axis=1, keepdims=True)

    rows_n = E * per_slot
    carry = gate_up(h, (jnp.zeros((rows_n, 2 * FB), wide), jnp.zeros((rows_n, 1), wide)))

    def next_cols(i, carry):
        at = (h + T - i) % T
        rows_copy(at, h).wait_recv()
        return gate_up(at, carry)

    total, squares = lax.fori_loop(1, T, next_cols, carry)
    total = total * lax.rsqrt(squares / D + epsilon)
    hidden = (jax.nn.silu(total[:, :FB]) * total[:, FB:]).astype(narrow)

    in_slices(hidden, wdn_v, down_send)
    to_plane(down_send, down_recv, 3)
    down_recv[h] = down_send[h]
    whole_wait(disp_send, E - 1, phase_send.at[1])
    whole_wait(rows_all, T - 1, phase_send.at[2])
    whole_wait(down_recv, T - 1, phase_recv.at[3])
    expert_out = functools.reduce(jnp.add, [down_recv[i].astype(wide) for i in range(T)])
    expert_out = expert_out.astype(narrow).astype(wide)

    for r in range(per_slot):
        ret_send[:, r, :] = expert_out[r * E : (r + 1) * E]
    to_column(ret_send, ret_recv, 4)
    ret_recv[e] = ret_send[e]
    whole_wait(down_send, T - 1, phase_send.at[3])
    for ch in whole:
        peer_copy(0, z, 0, ch, own_rows).wait_send()
        for d in (0, 1):
            for s in range(1, half):
                ring_copy(d, z, s, ch).wait_send()
                peer_copy(d, z, s, ch, own_rows).wait_send()
            if ch in dirs[d][2]:
                ring_copy(d, z, half, ch).wait_send()
                peer_copy(d, z, half, ch, own_rows).wait_send()
    whole_wait(ret_recv, E - 1, phase_recv.at[4])
    result = mixed_v[...]
    for r in range(per_slot):
        result += jnp.dot(
            picked[r] * weight,
            ret_recv[:, r, :],
            preferred_element_type=wide,
            precision=lax.Precision.HIGHEST,
        )
    out[...] = result.astype(narrow)
    whole_wait(ret_send, E - 1, phase_send.at[4])


def on_device(E, T, *args):
    (
        tokens,
        norm_gain,
        w_query,
        w_key,
        w_decay,
        w_value,
        w_outgate,
        decay_rate,
        state,
        head_gain,
        w_output,
        moe_gain,
        expert_ids,
        group_prob,
        inner_prob,
        w_gate,
        w_up,
        w_down,
    ) = args
    S, D = tokens.shape
    KB, QC = w_query.shape
    VC = w_value.shape[1]
    FB = w_down.shape[1]
    CW = D // T
    Z = E // 2
    steps = Z // 2 + 1
    slots = max(2, S * expert_ids.shape[1] // E)
    vmem = pl.BlockSpec(memory_space=pltpu.VMEM)
    hbm = pl.BlockSpec(memory_space=pl.ANY)
    cols = 3 * QC + 2 * VC
    dma = pltpu.SemaphoreType.DMA
    return pl.pallas_call(
        functools.partial(kernel, E, T),
        out_shape=jax.ShapeDtypeStruct((S, CW), narrow),
        in_specs=[vmem, vmem, hbm, hbm, hbm, hbm, hbm, vmem, hbm, vmem, hbm]
        + [vmem, vmem, vmem, vmem, hbm, hbm, hbm],
        out_specs=vmem,
        scratch_shapes=[
            pltpu.VMEM((Z, 2 * KB, cols), narrow),
            pltpu.VMEM((Z, S, 2 * KB), narrow),
            pltpu.VMEM((S, cols), wide),
            pltpu.VMEM((S, QC, VC), wide),
            pltpu.VMEM((VC, D), narrow),
            pltpu.VMEM((D, 2 * FB), narrow),
            pltpu.VMEM((FB, D), narrow),
            pltpu.VMEM((T, S, CW), narrow),
            pltpu.VMEM((T, S, CW), narrow),
            pltpu.VMEM((E, slots, CW), wide),
            pltpu.VMEM((E, slots, CW), wide),
            pltpu.VMEM((T, E * slots, CW), narrow),
            pltpu.VMEM((T, E * slots, CW), narrow),
            pltpu.VMEM((T, E * slots, CW), narrow),
            pltpu.VMEM((E, slots, CW), wide),
            pltpu.VMEM((E, slots, CW), wide),
            pltpu.VMEM((S, CW), wide),
            dma((5,)),
            dma((5,)),
            dma((2, steps, 4)),
            dma((2, steps, 4)),
            dma((2, steps, 4)),
            dma((2, steps, 4)),
            dma((5,)),
            dma((5,)),
            dma((T,)),
        ],
        compiler_params=pltpu.CompilerParams(
            collective_id=0, has_side_effects=True, vmem_limit_bytes=60 * 1024 * 1024
        ),
    )(
        tokens,
        norm_gain.reshape(1, D),
        w_query,
        w_key,
        w_decay,
        w_value,
        w_outgate,
        decay_rate.reshape(1, QC),
        state.reshape(S, QC, VC),
        head_gain.reshape(1, VC),
        w_output,
        moe_gain.reshape(1, D),
        expert_ids,
        group_prob.reshape(S, 1),
        inner_prob,
        w_gate.reshape(D, FB),
        w_up.reshape(D, FB),
        w_down.reshape(FB, D),
    )


def solution(mesh):
    placed = (
        P("ep", None),
        P(),
        P("ep", "tp"),
        P("ep", "tp"),
        P("ep", "tp"),
        P("ep", "tp"),
        P("ep", "tp"),
        P("tp"),
        P("ep", "tp", None, None),
        P(),
        P("tp", None),
        P(),
        P("ep", None),
        P("ep"),
        P("ep", None),
        P("ep", None, "tp"),
        P("ep", None, "tp"),
        P("ep", "tp", None),
    )
    return jax.shard_map(
        functools.partial(on_device, mesh.shape["ep"], mesh.shape["tp"]),
        mesh=mesh,
        in_specs=placed,
        out_specs=P("ep", "tp"),
        check_vma=False,
    )
```
